32 devices in a mesh: ep: 4 (over y, x), tp: 8 (over z, core).
Axes of the slice: x: 2, y: 2, z: 4, core: 2. Of those that a mesh axis runs over, the one named last changes fastest.
Arguments:
- tokens: bfloat16 [768, 4096], P('ep', 'tp'), may hold values from -60 to 60
- norm_gain: float32 [4096], P('tp'), may hold values from 0.1 to 1.9
- norm_bias: float32 [4096], P('tp'), may hold values from -3 to 3
- expert_ids: int32 [768, 2], P('ep'), may hold values from 0 to 15, all different within a row; in each aligned block of 192 rows (0 to 191, 192 to 383, ...) at most 48 rows name the same one
- route_weights: float32 [768, 2], P('ep'), may hold values from 0.1 to 1
- gate_weight: bfloat16 [16, 4096, 4096], P('ep', None, 'tp'), may hold values from -0.375 to 0.375
- up_weight: bfloat16 [16, 4096, 4096], P('ep', None, 'tp'), may hold values from -0.375 to 0.375
- down_weight: bfloat16 [16, 4096, 4096], P('ep', None, 'tp'), may hold values from -0.01171875 to 0.01171875
Outputs:
- combined: bfloat16 [768, 4096], P('ep', 'tp')
The draws below stay inside these ranges and needn't reach their ends.
Inputs may be any that keep to these rules, and one draw needn't show every extreme that they name: `expert_ids`: each row names 2 different experts. Among the 192 rows of one index of ep (aligned blocks of 192 rows), no expert is named more than 48 times, a bound that some block reaches.
All inputs are finite; a program needn't handle non-finite values.
Results may differ from the reference program's by a relative error of at most 0.0071.
Values may be sent and summed in bfloat16 or wider, within the bound.
A program may use at most 128 MiB of HBM per device.

```python
import math
import jax
import jax.numpy as jnp
import numpy as np
from jax import lax

D = 4096
FF = 4096
EXPERTS = 16
TOP = 2
TOK_DEV = 192
CAP = 48
TOKENS = 768
N_EP = 4


def draw_tokens(key, part):
    key_base = jax.random.fold_in(key, 11)
    key_column = jax.random.fold_in(key, 12)
    column_scale = jnp.exp(jnp.linspace(0.0, math.log(4.0), D)) * jax.random.uniform(key_column, (D,), jnp.float32, 0.5, 1.5)
    base_draw = jax.random.normal(key_base, (TOKENS, D), jnp.float32)
    values = base_draw * column_scale
    return jnp.clip(values, -60.0, 60.0).astype(jnp.bfloat16)


def shard_levels(own_key, extent, shards, smallest, high):
    level = 1.0
    for axis_at, shards_of in shards:
        heights = jax.random.uniform(jax.random.fold_in(jax.random.fold_in(own_key, 6), axis_at), (shards_of,), jnp.float32, smallest / len(shards), high / len(shards))
        level = level * jnp.repeat(jnp.exp(heights), extent[axis_at] // shards_of).reshape((-1,) + (1,) * (len(extent) - 1 - axis_at))
    return level


def shared_out(key, own, number, rows, number_of, top, bound, skew):
    ranking = jax.random.permutation(key, number_of)
    packed, usual = portions_of(number_of, rows * top, bound, skew, True), portions_of(number_of, rows * top, bound, skew, False)
    places = jnp.arange(number_of)

    def named(lengths, offset_by):
        used = int((lengths > 0).sum())
        fixed = max(1, used // 4)
        shifted = fixed + (places - fixed + offset_by * (used - fixed)) % max(1, number_of - fixed)
        return jnp.zeros((number_of,), jnp.int32).at[ranking[jnp.where(places < fixed, places, shifted)]].set(jnp.asarray(lengths, jnp.int32))

    lengths = jnp.where(number % 4 == 0, named(packed, number // 4), named(usual, number - number // 4 - 1))
    mixed = jax.random.permutation(jax.random.fold_in(own, 3), number_of)
    giver, receiver = mixed[0:number_of // 2 * 2:2], mixed[1:number_of // 2 * 2:2]
    slack = jnp.minimum(lengths[giver] - 1, bound - lengths[receiver]) // 2
    slack = jnp.where((giver == ranking[0]) | (receiver == ranking[0]) | (lengths[receiver] == 0), 0, jnp.maximum(slack, 0))
    shifted = jax.random.randint(jax.random.fold_in(own, 4), (number_of // 2,), 0, 1 << 20) % (slack + 1)
    lengths = lengths.at[giver].add(-shifted).at[receiver].add(shifted)
    items = jnp.searchsorted(jnp.cumsum(lengths), jnp.arange(rows * top), side="right").astype(jnp.int32)
    grid = items.reshape(top, rows).T
    grid = grid[jax.random.permutation(jax.random.fold_in(own, 1), rows)]
    offset_by = jax.random.randint(jax.random.fold_in(own, 2), (rows, 1), 0, top)
    return jnp.take_along_axis(grid, (jnp.arange(top)[None, :] + offset_by) % top, axis=1)


def portions_of(amount, total, reach, slope, full):
    portions = [(1 << 20) // math.isqrt(rank ** slope) + 1 for rank in range(1, amount + 1)]
    largest = reach if full else min(reach, max(-(-total // amount), total * portions[0] // sum(portions)))
    least = 1 if total - largest >= amount - 1 else 0
    holding, rest = [largest] + [least] * (amount - 1), total - largest - least * (amount - 1)
    while rest > 0:
        candidates = [i for i in range(1, amount) if holding[i] < largest] or [i for i in range(1, amount) if holding[i] < reach]
        pool, left = sum([portions[i] for i in candidates]), rest
        for i in candidates:
            more = min(reach - holding[i], max(1, left * portions[i] // pool), rest)
            holding[i] = holding[i] + more
            rest = rest - more
    return np.array(holding)


def normal_values(stream_key, extent, scale, bound, cuts=(), held_as=jnp.bfloat16):
    entries = scale * jax.random.normal(stream_key, extent, jnp.float32)
    if cuts:
        entries = entries * shard_levels(stream_key, extent, cuts, -0.22, 0.18)
    return jnp.clip(entries, -bound, bound).astype(held_as)


def setup_inputs(seed: int = 0) -> dict:
    arg_keys = jax.random.split(jax.random.key(seed), 9)
    tokens = draw_tokens(jax.random.fold_in(arg_keys[8], 71), 0)
    norm_gain = jnp.clip(1.0 + 0.18 * jax.random.normal(arg_keys[1], (D,), jnp.float32), 0.1, 1.9)
    norm_bias = normal_values(arg_keys[2], (D,), 0.5, 3.0, ((0, 8),), jnp.float32)
    expert_ids_keys = jax.random.split(jax.random.fold_in(arg_keys[3], 1), TOKENS // TOK_DEV)
    expert_ids_turns = jax.random.permutation(jax.random.fold_in(arg_keys[3], 3), TOKENS // TOK_DEV)
    expert_ids = jax.vmap(lambda own, number: shared_out(jax.random.fold_in(arg_keys[3], 2), own, number, TOK_DEV, EXPERTS, TOP, CAP, 2))(expert_ids_keys, expert_ids_turns).reshape((TOKENS, TOP))
    route_weights = jnp.clip(0.1 + 0.9 * jax.random.uniform(arg_keys[4], (TOKENS, TOP), jnp.float32) ** shard_levels(arg_keys[4], (TOKENS, TOP), ((0, 4),), -0.2, 0.2), 0.1, 1.0)
    gate_weight = normal_values(arg_keys[5], (EXPERTS, D, FF), (D // 16) ** -0.5, 0.375, ((0, 4), (2, 8)))
    up_weight = normal_values(arg_keys[6], (EXPERTS, D, FF), (D // 16) ** -0.5, 0.375, ((0, 4), (2, 8)))
    down_weight = normal_values(arg_keys[7], (EXPERTS, FF, D), (64 * FF) ** -0.5, 0.01171875, ((0, 4), (2, 8)))
    return {"tokens": tokens, "norm_gain": norm_gain, "norm_bias": norm_bias, "expert_ids": expert_ids, "route_weights": route_weights, "gate_weight": gate_weight, "up_weight": up_weight, "down_weight": down_weight}


clamp_limit = 7.0
swish_alpha = 1.702
norm_epsilon = 1e-05

def clamped_unit(gate_pre, up_pre):
    gate_cut = jnp.minimum(gate_pre, clamp_limit)
    up_cut = jnp.clip(up_pre, -clamp_limit, clamp_limit)
    return gate_cut * jax.nn.sigmoid(swish_alpha * gate_cut) * (up_cut + 1.0)

def reference(tokens, norm_gain, norm_bias, expert_ids, route_weights, gate_weight, up_weight, down_weight):
    values = tokens.astype(jnp.float32)
    average = lax.optimization_barrier(jnp.sum(values, 1)) / D
    spread = lax.optimization_barrier(jnp.sum(values * values, 1)) / D - average * average
    normed = ((values - average[:, None]) * lax.rsqrt(spread + norm_epsilon)[:, None] * norm_gain + norm_bias).astype(jnp.bfloat16)
    flat_ids = expert_ids.reshape(-1).astype(jnp.int32)
    blocks = flat_ids.reshape(N_EP, TOK_DEV * TOP)
    onehot = (blocks[:, :, None] == jnp.arange(EXPERTS, dtype=jnp.int32)).astype(jnp.int32)
    slot_rank = lax.optimization_barrier(jnp.sum((jnp.cumsum(onehot, 1) - onehot) * onehot, -1)).reshape(-1)
    source = jnp.arange(TOKENS * TOP, dtype=jnp.int32) // (TOK_DEV * TOP)
    target = (flat_ids * N_EP + source) * CAP + slot_rank
    source_row = jnp.full((EXPERTS * N_EP * CAP,), TOKENS, jnp.int32).at[target].set(jnp.arange(TOKENS * TOP, dtype=jnp.int32) // TOP)
    padded = jnp.concatenate([normed, jnp.zeros((1, D), jnp.bfloat16)], 0)

    def one_expert(operand):
        row_index, gate_rows, up_rows, down_rows = operand
        routed = padded[row_index]
        gate_pre = jnp.dot(routed, gate_rows, preferred_element_type=jnp.float32)
        up_pre = jnp.dot(routed, up_rows, preferred_element_type=jnp.float32)
        hidden = clamped_unit(gate_pre, up_pre).astype(jnp.bfloat16)
        return jnp.dot(hidden, down_rows, preferred_element_type=jnp.float32).astype(jnp.bfloat16)
    results = lax.map(one_expert, (source_row.reshape(EXPERTS, N_EP * CAP), gate_weight, up_weight, down_weight))
    picked = results.reshape(-1, D)[target].reshape(TOKENS, TOP, D).astype(jnp.float32)
    return lax.optimization_barrier(jnp.sum(picked * route_weights[:, :, None], 1)).astype(jnp.bfloat16)
```

```python
import functools
import math

import jax
import jax.numpy as jnp
from jax import lax
from jax.experimental import pallas as pl
from jax.experimental.pallas import tpu as pltpu
from jax.sharding import PartitionSpec as P

CAP = 48
SPLIT = 2
LAG = 2
MESH = pl.DeviceIdType.MESH

clamp_limit = 7.0
swish_alpha = 1.702
norm_epsilon = 1e-05


def clamped_unit(gate_pre, up_pre):
    gate_cut = jnp.minimum(gate_pre, clamp_limit)
    up_cut = jnp.clip(up_pre, -clamp_limit, clamp_limit)
    return gate_cut * jax.nn.sigmoid(swish_alpha * gate_cut) * (up_cut + 1.0)


def remote(src, dst, send_sem, recv_sem, device):
    return pltpu.make_async_remote_copy(
        src_ref=src,
        dst_ref=dst,
        send_sem=send_sem,
        recv_sem=recv_sem,
        device_id=device,
        device_id_type=MESH,
    )


def layer_kernel(
    side, n_tp, top,
    x_ref, gain_ref, bias_ref, ids_ref, rw_ref, gate_hbm, up_hbm, down_hbm,
    o_ref,
    tok, own_meta, meta, gains, biases, upper, wg, wu, wd, normed, routed, hid, res,
    part, ret_out, ret_in,
    w_sem, d_sem, own_sem, t_send, o_send, y_send, t_recv, g_send, g_recv, m_send, m_recv,
    h_send, h_recv, r_send, r_recv,
):
    rows, columns = x_ref.shape
    width = columns * n_tp
    local = wg.shape[0]
    chips, n_ep = n_tp // 2, side * side
    pieces = n_ep * local
    half = rows // SPLIT
    shift = local // 2
    e, t = lax.axis_index("ep"), lax.axis_index("tp")
    z, c = t // 2, t % 2
    ey, ex = e // side, e % side
    partner = z * 2 + 1 - c
    right, left = (e, t + 2), (e, t - 2)
    row_peers = [ey * side + (ex + i) % side for i in range(1, side)]
    column_peers = [((ey + i) % side) * side + ex for i in range(1, side)]
    far = [
        ((ey + j) % side) * side + (ex + i) % side
        for j in range(1, side)
        for i in range(1, side)
    ]

    def source(p):
        return ((ey + p // side) % side) * side + (ex + p % side) % side

    def cols(tt):
        return pl.ds(pl.multiple_of(tt * columns, columns), columns)

    def load_in(j):
        return (
            pltpu.make_async_copy(gate_hbm.at[j], wg.at[j], w_sem.at[0, j]),
            pltpu.make_async_copy(up_hbm.at[j], wu.at[j], w_sem.at[1, j]),
        )

    def piece_of(i):
        return (i + shift) % pieces

    def load_down(i):
        return pltpu.make_async_copy(
            down_hbm.at[piece_of(i) % local], wd.at[i % 2], d_sem.at[i % 2]
        )

    for i in range(local):
        for copy in load_in((i + shift) % local):
            copy.start()

    barrier = pltpu.get_barrier_semaphore()
    for i in range(1, n_tp):
        pl.semaphore_signal(barrier, inc=1, device_id=(e, (t + i) % n_tp), device_id_type=MESH)
    for i in range(1, n_ep):
        pl.semaphore_signal(barrier, inc=1, device_id=((e + i) % n_ep, t), device_id_type=MESH)

    a = lax.broadcasted_iota(jnp.int32, (rows, rows), 0)
    b = lax.broadcasted_iota(jnp.int32, (rows, rows), 1)
    upper[...] = (a < b).astype(jnp.float32).astype(jnp.bfloat16)
    for k in range(top):
        named = ids_ref[:, k : k + 1].astype(jnp.float32)
        own_meta[k : k + 1, :] = jnp.sum(jnp.where(a == b, named, 0.0), 0, keepdims=True)
        held = rw_ref[:, k : k + 1]
        own_meta[top + k : top + k + 1, :] = jnp.sum(
            jnp.where(a == b, held, 0.0), 0, keepdims=True
        )
    pl.semaphore_wait(barrier, n_tp - 1 + n_ep - 1)

    def lines(q):
        return pl.ds(q * half, half)

    def block(s, q, zz):
        return tok.at[s, lines(q), cols(zz * 2 + c)]

    def send(src, s, q, zz, sem, device):
        return remote(src, block(s, q, zz), sem, t_recv.at[s, q, zz * 2 + c], device)

    def to_partner(src, s, q, zz):
        return send(src, s, q, zz, t_send.at[s, q, zz], (e, partner))

    def along(src, q, zz, kind):
        return send(src, e, q, zz, o_send.at[q, zz, kind], (right, left)[kind])

    def arrived(s, q, zz):
        to_partner(block(s, q, zz), s, q, zz).wait_recv()

    def own_out(src, q, zz):
        return [
            send(src, e, q, zz, o_send.at[q, zz, 2 + i], (s, t))
            for i, s in enumerate(row_peers + column_peers)
        ] + [to_partner(src, e, q, zz)]

    def relayed(i, s, targets, q, zz):
        return [
            send(block(s, q, zz), s, q, zz, y_send.at[i, q, zz, n], (o, t))
            for n, o in enumerate(targets)
        ]

    def out(src, q, zz):
        for copy in own_out(src, q, zz):
            copy.start()

    own = []
    for q in range(SPLIT):
        src = x_ref.at[lines(q), :]

        @pl.when(z < chips - 1)
        def _():
            along(src, q, z, 0).start()

        @pl.when(z > 0)
        def _():
            along(src, q, z, 1).start()

        out(src, q, z)
        own.append(pltpu.make_async_copy(src, block(e, q, z), own_sem.at[q]))
        own[-1].start()

    gb_own = [
        pltpu.make_async_copy(gain_ref, gains.at[:, cols(t)], own_sem.at[SPLIT]),
        pltpu.make_async_copy(bias_ref, biases.at[:, cols(t)], own_sem.at[SPLIT + 1]),
        pltpu.make_async_copy(own_meta, meta.at[e], own_sem.at[SPLIT + 2]),
    ]
    for copy in gb_own:
        copy.start()

    def gb_copy(n, ref, dst, i, o):
        return remote(ref, dst.at[:, cols(o)], g_send.at[n, i], g_recv.at[n, o], (e, (t + i) % n_tp))

    def meta_copy(i, o):
        return remote(own_meta, meta.at[o], m_send.at[i], m_recv.at[o], ((e + i) % n_ep, t))

    for i in range(1, n_tp):
        gb_copy(0, gain_ref, gains, i, t).start()
        gb_copy(1, bias_ref, biases, i, t).start()
    for i in range(1, n_ep):
        meta_copy(i, e).start()
    load_down(0).start()
    load_down(1).start()

    def line_round(k):
        for q in range(SPLIT):

            @pl.when(z - k >= 0)
            def _():
                zz = z - k
                arrived(e, q, zz)

                @pl.when(z < chips - 1)
                def _():
                    along(block(e, q, zz), q, zz, 0).start()

                out(block(e, q, zz), q, zz)

            @pl.when(z + k < chips)
            def _():
                zz = z + k
                arrived(e, q, zz)

                @pl.when(z > 0)
                def _():
                    along(block(e, q, zz), q, zz, 1).start()

                out(block(e, q, zz), q, zz)

    def both(k, act):
        if k == 0:
            act(z)
        else:

            @pl.when(z - k >= 0)
            def _():
                act(z - k)

            @pl.when(z + k < chips)
            def _():
                act(z + k)

    def relay(zz):
        for q in range(SPLIT):
            for parity, peers, targets in (
                (0, row_peers, column_peers), (1, column_peers, row_peers)
            ):
                for i, s in enumerate(peers):
                    arrived(s, q, zz)

                    @pl.when(zz % 2 == parity)
                    def _():
                        for copy in relayed(i, s, targets, q, zz):
                            copy.start()

                    to_partner(block(s, q, zz), s, q, zz).start()

    def last(zz):
        for q in range(SPLIT):
            for s in far:
                arrived(s, q, zz)
                to_partner(block(s, q, zz), s, q, zz).start()

    early = max(0, chips - 3)
    for k in range(1, chips):
        line_round(k)
        if k >= 2 and k - 2 < early:
            both(k - 2, relay)
    for copy in own + gb_own:
        copy.wait()
    for i in range(1, n_tp):
        o = (t + i) % n_tp
        gb_copy(0, gain_ref, gains, i, o).wait_recv()
        gb_copy(1, bias_ref, biases, i, o).wait_recv()
    for i in range(1, n_ep):
        meta_copy(i, (e + i) % n_ep).wait_recv()

    def from_partner(s):
        for zz in range(chips):
            for q in range(SPLIT):
                other = tok.at[s, lines(q), cols(zz * 2 + 1 - c)]
                remote(
                    other, other, t_send.at[s, q, zz],
                    t_recv.at[s, q, zz * 2 + 1 - c], (e, partner),
                ).wait_recv()

    step_rows = 32 if rows % 32 == 0 else 16

    def normalise(s, slot):
        def body(r, carry):
            at = pl.ds(pl.multiple_of(r * step_rows, step_rows), step_rows)
            total = jnp.zeros((step_rows, 128), jnp.float32)
            squares = jnp.zeros((step_rows, 128), jnp.float32)
            for k in range(width // 128):
                v = tok[s, at, k * 128 : (k + 1) * 128].astype(jnp.float32)
                total = total + v
                squares = squares + v * v
            average = jnp.sum(total, 1, keepdims=True) / width
            spread = jnp.sum(squares, 1, keepdims=True) / width - average * average
            factor = jnp.broadcast_to(lax.rsqrt(spread + norm_epsilon), (step_rows, 128))
            average = jnp.broadcast_to(average, (step_rows, 128))
            for k in range(width // 128):
                here = slice(k * 128, (k + 1) * 128)
                v = tok[s, at, here].astype(jnp.float32)
                v = (v - average) * factor * gains[:, here] + biases[:, here]
                normed[slot, at, here] = v.astype(jnp.bfloat16)
            return carry

        lax.fori_loop(0, rows // step_rows, body, 0)

    def chosen(s, j):
        ids = [meta[s, k : k + 1, :] for k in range(top)]
        expert = (e * local + j).astype(jnp.float32)
        hits = [(row == expert).astype(jnp.float32) for row in ids]
        hit = functools.reduce(jnp.add, hits)
        wide = jnp.broadcast_to(hit, (16, rows)).astype(jnp.bfloat16)
        rank = jnp.dot(wide, upper[...], preferred_element_type=jnp.float32)[:1]
        line = lax.broadcasted_iota(jnp.int32, (CAP, rows), 0).astype(jnp.float32)
        match = jnp.where(line == rank, jnp.broadcast_to(hit, (CAP, rows)), 0.0)
        return match, hits

    def weights_of(s, j):
        match, hits = chosen(s, j)
        held = functools.reduce(
            jnp.add, [hits[k] * meta[s, top + k : top + k + 1, :] for k in range(top)]
        )
        return match * held

    def hid_block(u, zz):
        return hid.at[u, :, cols(zz * 2 + c)]

    def h_copy(u, zz, kind, device):
        return remote(
            hid_block(u, zz), hid_block(u, zz),
            h_send.at[u, zz, kind], h_recv.at[u, zz * 2 + c], device,
        )

    def compute(u):
        p, j = u // local, u % local
        s = source(p)
        slot = jnp.minimum(p, 1)
        match, _ = chosen(s, j)
        match = match.astype(jnp.bfloat16)
        wide = min(512, width)

        def pick(k, carry):
            here = pl.ds(pl.multiple_of(k * wide, wide), wide)
            routed[:, here] = jnp.dot(
                match, normed[slot, :, here], preferred_element_type=jnp.float32
            ).astype(jnp.bfloat16)
            return carry

        lax.fori_loop(0, width // wide, pick, 0)
        gate = jnp.dot(routed[...], wg[j], preferred_element_type=jnp.float32)
        up = jnp.dot(routed[...], wu[j], preferred_element_type=jnp.float32)
        hid[u, :, cols(t)] = clamped_unit(gate, up).astype(jnp.bfloat16)

        @pl.when(z < chips - 1)
        def _():
            h_copy(u, z, 1, right).start()

        @pl.when(z > 0)
        def _():
            h_copy(u, z, 2, left).start()

        h_copy(u, z, 0, (e, partner)).start()

    def hidden_round(u, k):
        @pl.when(z - k >= 0)
        def _():
            zz = z - k
            h_copy(u, zz, 0, (e, partner)).wait_recv()

            @pl.when(z < chips - 1)
            def _():
                h_copy(u, zz, 1, right).start()

            h_copy(u, zz, 0, (e, partner)).start()

        @pl.when(z + k < chips)
        def _():
            zz = z + k
            h_copy(u, zz, 0, (e, partner)).wait_recv()

            @pl.when(z > 0)
            def _():
                h_copy(u, zz, 2, left).start()

            h_copy(u, zz, 0, (e, partner)).start()

    def hidden_full(u):
        for zz in range(chips):
            other = hid.at[u, :, cols(zz * 2 + 1 - c)]
            remote(
                other, other, h_send.at[u, zz, 0], h_recv.at[u, zz * 2 + 1 - c], (e, partner)
            ).wait_recv()

    def combine(p):
        s = source(p)
        mix = [weights_of(s, j) for j in range(local)]
        mix = mix[0] if local == 1 else jnp.concatenate(mix, 0)
        high = mix.astype(jnp.bfloat16)
        low = (mix - high.astype(jnp.float32)).astype(jnp.bfloat16)
        dims = (((0,), (0,)), ((), ()))
        outs = res[p]
        part[...] = lax.dot_general(
            high, outs, dims, preferred_element_type=jnp.float32
        ) + lax.dot_general(low, outs, dims, preferred_element_type=jnp.float32)

    def ret_copy(p, s, o):
        return remote(ret_out.at[p], ret_in.at[o], r_send.at[p], r_recv.at[o], (s, t))

    def down(i):
        u = piece_of(i)
        p, j = u // local, u % local
        hidden_full(u)
        load_down(i).wait()
        made = jnp.dot(hid[u], wd[i % 2], preferred_element_type=jnp.float32)
        res[p, pl.ds(pl.multiple_of(j * CAP, CAP), CAP), :] = made.astype(jnp.bfloat16)

        @pl.when(i + 2 < pieces)
        def _():
            load_down(i + 2).start()

        @pl.when((p > 0) & (j == local - 1))
        def _():
            combine(p)
            ret_out[p] = part[...].astype(jnp.bfloat16)
            ret_copy(p, source(p), e).start()

    lead = (chips - 1) * LAG + 1
    first_other = local - shift
    first_far = (side + 1) * local - shift
    relays = [(min(k - early, first_other - 1), k) for k in range(early, chips)]
    lasts = [(max(first_far - chips + k, first_other - 1), k) for k in range(chips)]

    def step(i, carry):
        @pl.when(i < pieces)
        def _():
            u = piece_of(i)
            p, j = u // local, u % local

            @pl.when(((j == 0) & (p > 0)) | (i == 0))
            def _():
                s = source(p)
                from_partner(s)
                normalise(s, jnp.minimum(p, 1))

            @pl.when(i < local)
            def _():
                for copy in load_in(j):
                    copy.wait()

            compute(u)

        for k in range(1, chips):
            ii = i - k * LAG

            @pl.when((ii >= 0) & (ii < pieces))
            def _():
                hidden_round(piece_of(ii), k)

        for act, places in ((relay, relays), (last, lasts)):
            for at in sorted({place for place, _ in places}):

                @pl.when(i == at)
                def _():
                    for place, k in places:
                        if place == at:
                            both(k, act)

        @pl.when(i >= lead)
        def _():
            down(i - lead)

        return carry

    lax.fori_loop(0, pieces + lead, step, 0)

    combine(0)
    total = part[...]
    for i in range(1, n_ep):
        o = (e + i) % n_ep
        ret_copy(i, o, o).wait_recv()
        total = total + ret_in[o].astype(jnp.float32)
    o_ref[...] = total.astype(jnp.bfloat16)

    for p in range(1, n_ep):
        ret_copy(p, source(p), e).wait_send()
        meta_copy(p, e).wait_send()
    for i in range(1, n_tp):
        gb_copy(0, gain_ref, gains, i, t).wait_send()
        gb_copy(1, bias_ref, biases, i, t).wait_send()
    for q in range(SPLIT):
        for zz in range(chips):
            for s in range(n_ep):
                to_partner(block(s, q, zz), s, q, zz).wait_send()

            @pl.when((zz <= z) & (z < chips - 1))
            def _():
                along(block(e, q, zz), q, zz, 0).wait_send()

            @pl.when((zz >= z) & (z > 0))
            def _():
                along(block(e, q, zz), q, zz, 1).wait_send()

            for copy in own_out(block(e, q, zz), q, zz)[:-1]:
                copy.wait_send()
            peers, targets = (row_peers, column_peers)[:: 1 - 2 * (zz % 2)]
            for i, s in enumerate(peers):
                for copy in relayed(i, s, targets, q, zz):
                    copy.wait_send()

    def sent(u, carry):
        for zz in range(chips):
            h_copy(u, zz, 0, (e, partner)).wait_send()

            @pl.when((zz <= z) & (z < chips - 1))
            def _():
                h_copy(u, zz, 1, right).wait_send()

            @pl.when((zz >= z) & (z > 0))
            def _():
                h_copy(u, zz, 2, left).wait_send()

        return carry

    lax.fori_loop(0, pieces, sent, 0)


def on_device(
    n_ep, n_tp,
    tokens, norm_gain, norm_bias, expert_ids, route_weights, gate_weight, up_weight, down_weight,
):
    rows, columns = tokens.shape
    top = expert_ids.shape[1]
    local = gate_weight.shape[0]
    side = math.isqrt(n_ep)
    chips = n_tp // 2
    width = columns * n_tp
    pieces = n_ep * local
    vmem = pl.BlockSpec(memory_space=pltpu.VMEM)
    anywhere = pl.BlockSpec(memory_space=pl.ANY)
    bf16, f32, dma = jnp.bfloat16, jnp.float32, pltpu.SemaphoreType.DMA
    return pl.pallas_call(
        functools.partial(layer_kernel, side, n_tp, top),
        out_shape=jax.ShapeDtypeStruct((rows, columns), bf16),
        in_specs=[vmem] * 5 + [anywhere] * 3,
        out_specs=vmem,
        scratch_shapes=[
            pltpu.VMEM((n_ep, rows, width), bf16),
            pltpu.VMEM((8, rows), f32),
            pltpu.VMEM((n_ep, 8, rows), f32),
            pltpu.VMEM((1, width), f32),
            pltpu.VMEM((1, width), f32),
            pltpu.VMEM((rows, rows), bf16),
            pltpu.VMEM((local, width, columns), bf16),
            pltpu.VMEM((local, width, columns), bf16),
            pltpu.VMEM((2, width, columns), bf16),
            pltpu.VMEM((2, rows, width), bf16),
            pltpu.VMEM((CAP, width), bf16),
            pltpu.VMEM((pieces, CAP, width), bf16),
            pltpu.VMEM((n_ep, local * CAP, columns), bf16),
            pltpu.VMEM((rows, columns), f32),
            pltpu.VMEM((n_ep, rows, columns), bf16),
            pltpu.VMEM((n_ep, rows, columns), bf16),
            dma((2, local)),
            dma((2,)),
            dma((SPLIT + 3,)),
            dma((n_ep, SPLIT, chips)),
            dma((SPLIT, chips, 2 * side)),
            dma((side - 1, SPLIT, chips, side - 1)),
            dma((n_ep, SPLIT, n_tp)),
            dma((2, n_tp)),
            dma((2, n_tp)),
            dma((n_ep,)),
            dma((n_ep,)),
            dma((pieces, chips, 3)),
            dma((pieces, n_tp)),
            dma((n_ep,)),
            dma((n_ep,)),
        ],
        compiler_params=pltpu.CompilerParams(
            collective_id=0, has_side_effects=True, vmem_limit_bytes=66_000_000
        ),
    )(
        tokens, norm_gain.reshape(1, columns), norm_bias.reshape(1, columns),
        expert_ids, route_weights, gate_weight, up_weight, down_weight,
    )


def solution(mesh):
    n_ep, n_tp = mesh.shape["ep"], mesh.shape["tp"]
    placed = (
        P("ep", "tp"),
        P("tp"),
        P("tp"),
        P("ep", None),
        P("ep", None),
        P("ep", None, "tp"),
        P("ep", None, "tp"),
        P("ep", None, "tp"),
    )
    return jax.shard_map(
        functools.partial(on_device, n_ep, n_tp),
        mesh=mesh,
        in_specs=placed,
        out_specs=P("ep", "tp"),
        check_vma=False,
    )
```

```python
import functools
import math

import jax
import jax.numpy as jnp
from jax import lax
from jax.experimental import pallas as pl
from jax.experimental.pallas import tpu as pltpu
from jax.sharding import PartitionSpec as P

CAP = 48
SPLIT = 2
LAG = 2
SHIFT = 1
PICK = 1024
MESH = pl.DeviceIdType.MESH

clamp_limit = 7.0
swish_alpha = 1.702
norm_epsilon = 1e-05


def clamped_unit(gate_pre, up_pre):
    gate_cut = jnp.minimum(gate_pre, clamp_limit)
    up_cut = jnp.clip(up_pre, -clamp_limit, clamp_limit)
    return gate_cut * jax.nn.sigmoid(swish_alpha * gate_cut) * (up_cut + 1.0)


def remote(src, dst, send_sem, recv_sem, device):
    return pltpu.make_async_remote_copy(
        src_ref=src,
        dst_ref=dst,
        send_sem=send_sem,
        recv_sem=recv_sem,
        device_id=device,
        device_id_type=MESH,
    )


def layer_kernel(
    side, n_tp, top,
    x_ref, gain_ref, bias_ref, ids_ref, rw_ref, gate_hbm, up_hbm, down_hbm,
    o_ref,
    tok, own_meta, meta, gains, biases, upper, wg, wu, wd, normed, routed, hid, res,
    part, ret_out, ret_in,
    w_sem, d_sem, own_sem, t_send, o_send, y_send, t_recv, g_send, g_recv, m_send, m_recv,
    h_send, h_recv, r_send, r_recv,
):
    rows, columns = x_ref.shape
    width = columns * n_tp
    local = wg.shape[0]
    chips, n_ep = n_tp // 2, side * side
    pieces = n_ep * local
    half = rows // SPLIT
    shift = min(SHIFT, local - 1)
    e, t = lax.axis_index("ep"), lax.axis_index("tp")
    z, c = t // 2, t % 2
    ey, ex = e // side, e % side
    partner = z * 2 + 1 - c
    right, left = (e, t + 2), (e, t - 2)
    row_peers = [ey * side + (ex + i) % side for i in range(1, side)]
    column_peers = [((ey + i) % side) * side + ex for i in range(1, side)]
    far = [
        ((ey + j) % side) * side + (ex + i) % side
        for j in range(1, side)
        for i in range(1, side)
    ]

    def source(p):
        return ((ey + p // side) % side) * side + (ex + p % side) % side

    def cols(tt):
        return pl.ds(pl.multiple_of(tt * columns, columns), columns)

    def load_in(j):
        return (
            pltpu.make_async_copy(gate_hbm.at[j], wg.at[j], w_sem.at[0, j]),
            pltpu.make_async_copy(up_hbm.at[j], wu.at[j], w_sem.at[1, j]),
        )

    def piece_of(i):
        return (i + shift) % pieces

    def load_down(i):
        return pltpu.make_async_copy(
            down_hbm.at[piece_of(i) % local], wd.at[i % 2], d_sem.at[i % 2]
        )

    for i in range(local):
        for copy in load_in((i + shift) % local):
            copy.start()

    barrier = pltpu.get_barrier_semaphore()
    for i in range(1, n_tp):
        pl.semaphore_signal(barrier, inc=1, device_id=(e, (t + i) % n_tp), device_id_type=MESH)
    for i in range(1, n_ep):
        pl.semaphore_signal(barrier, inc=1, device_id=((e + i) % n_ep, t), device_id_type=MESH)

    a = lax.broadcasted_iota(jnp.int32, (rows, rows), 0)
    b = lax.broadcasted_iota(jnp.int32, (rows, rows), 1)
    upper[...] = (a < b).astype(jnp.float32).astype(jnp.bfloat16)
    own_meta[:top, :] = ids_ref[...].astype(jnp.float32)
    own_meta[top : 2 * top, :] = rw_ref[...]
    pl.semaphore_wait(barrier, n_tp - 1 + n_ep - 1)

    def lines(q):
        return pl.ds(q * half, half)

    def block(s, q, zz):
        return tok.at[s, lines(q), cols(zz * 2 + c)]

    def send(src, s, q, zz, sem, device):
        return remote(src, block(s, q, zz), sem, t_recv.at[s, q, zz * 2 + c], device)

    def to_partner(src, s, q, zz):
        return send(src, s, q, zz, t_send.at[s, q, zz], (e, partner))

    def along(src, q, zz, kind):
        return send(src, e, q, zz, o_send.at[q, zz, kind], (right, left)[kind])

    def arrived(s, q, zz):
        to_partner(block(s, q, zz), s, q, zz).wait_recv()

    def own_out(src, q, zz):
        return [
            send(src, e, q, zz, o_send.at[q, zz, 2 + i], (s, t))
            for i, s in enumerate(row_peers + column_peers)
        ] + [to_partner(src, e, q, zz)]

    def relayed(i, s, targets, q, zz):
        return [
            send(block(s, q, zz), s, q, zz, y_send.at[i, q, zz, n], (o, t))
            for n, o in enumerate(targets)
        ]

    def out(src, q, zz):
        for copy in own_out(src, q, zz):
            copy.start()

    own = []
    for q in range(SPLIT):
        src = x_ref.at[lines(q), :]

        @pl.when(z < chips - 1)
        def _():
            along(src, q, z, 0).start()

        @pl.when(z > 0)
        def _():
            along(src, q, z, 1).start()

        out(src, q, z)
        own.append(pltpu.make_async_copy(src, block(e, q, z), own_sem.at[q]))
        own[-1].start()

    gb_own = [
        pltpu.make_async_copy(gain_ref, gains.at[:, cols(t)], own_sem.at[SPLIT]),
        pltpu.make_async_copy(bias_ref, biases.at[:, cols(t)], own_sem.at[SPLIT + 1]),
        pltpu.make_async_copy(own_meta, meta.at[e], own_sem.at[SPLIT + 2]),
    ]
    for copy in gb_own:
        copy.start()

    def gb_copy(n, ref, dst, i, o):
        return remote(ref, dst.at[:, cols(o)], g_send.at[n, i], g_recv.at[n, o], (e, (t + i) % n_tp))

    def meta_copy(i, o):
        return remote(own_meta, meta.at[o], m_send.at[i], m_recv.at[o], ((e + i) % n_ep, t))

    for i in range(1, n_tp):
        gb_copy(0, gain_ref, gains, i, t).start()
        gb_copy(1, bias_ref, biases, i, t).start()
    for i in range(1, n_ep):
        meta_copy(i, e).start()
    load_down(0).start()
    load_down(1).start()

    def line_round(k):
        for q in range(SPLIT):

            @pl.when(z - k >= 0)
            def _():
                zz = z - k
                arrived(e, q, zz)

                @pl.when(z < chips - 1)
                def _():
                    along(block(e, q, zz), q, zz, 0).start()

                out(block(e, q, zz), q, zz)

            @pl.when(z + k < chips)
            def _():
                zz = z + k
                arrived(e, q, zz)

                @pl.when(z > 0)
                def _():
                    along(block(e, q, zz), q, zz, 1).start()

                out(block(e, q, zz), q, zz)

    def both(k, act):
        if k == 0:
            act(z)
        else:

            @pl.when(z - k >= 0)
            def _():
                act(z - k)

            @pl.when(z + k < chips)
            def _():
                act(z + k)

    def relay(zz):
        for q in range(SPLIT):
            for parity, peers, targets in (
                (0, row_peers, column_peers), (1, column_peers, row_peers)
            ):
                for i, s in enumerate(peers):
                    arrived(s, q, zz)

                    @pl.when(zz % 2 == parity)
                    def _():
                        for copy in relayed(i, s, targets, q, zz):
                            copy.start()

                    to_partner(block(s, q, zz), s, q, zz).start()

    def last(zz):
        for q in range(SPLIT):
            for s in far:
                arrived(s, q, zz)
                to_partner(block(s, q, zz), s, q, zz).start()

    early = max(0, chips - 3)
    for k in range(1, chips):
        line_round(k)
        if k >= 2 and k - 2 < early:
            both(k - 2, relay)
    for copy in own + gb_own:
        copy.wait()
    for i in range(1, n_tp):
        o = (t + i) % n_tp
        gb_copy(0, gain_ref, gains, i, o).wait_recv()
        gb_copy(1, bias_ref, biases, i, o).wait_recv()
    for i in range(1, n_ep):
        meta_copy(i, (e + i) % n_ep).wait_recv()

    def from_partner(s):
        for zz in range(chips):
            for q in range(SPLIT):
                other = tok.at[s, lines(q), cols(zz * 2 + 1 - c)]
                remote(
                    other, other, t_send.at[s, q, zz],
                    t_recv.at[s, q, zz * 2 + 1 - c], (e, partner),
                ).wait_recv()

    step_rows = 32 if rows % 32 == 0 else 16

    def normalise(s):
        def body(r, carry):
            at = pl.ds(pl.multiple_of(r * step_rows, step_rows), step_rows)
            total = jnp.zeros((step_rows, 128), jnp.float32)
            squares = jnp.zeros((step_rows, 128), jnp.float32)
            for k in range(width // 128):
                v = tok[s, at, k * 128 : (k + 1) * 128].astype(jnp.float32)
                total = total + v
                squares = squares + v * v
            average = jnp.sum(total, 1, keepdims=True) / width
            spread = jnp.sum(squares, 1, keepdims=True) / width - average * average
            factor = jnp.broadcast_to(lax.rsqrt(spread + norm_epsilon), (step_rows, 128))
            average = jnp.broadcast_to(average, (step_rows, 128))
            for k in range(width // 128):
                here = slice(k * 128, (k + 1) * 128)
                v = tok[s, at, here].astype(jnp.float32)
                v = (v - average) * factor * gains[:, here] + biases[:, here]
                normed[at, here] = v.astype(jnp.bfloat16)
            return carry

        lax.fori_loop(0, rows // step_rows, body, 0)

    def chosen(s, j):
        ids = [meta[s, k : k + 1, :] for k in range(top)]
        expert = (e * local + j).astype(jnp.float32)
        hits = [(row == expert).astype(jnp.float32) for row in ids]
        hit = functools.reduce(jnp.add, hits)
        wide = jnp.broadcast_to(hit, (16, rows)).astype(jnp.bfloat16)
        rank = jnp.dot(wide, upper[...], preferred_element_type=jnp.float32)[:1]
        line = lax.broadcasted_iota(jnp.int32, (CAP, rows), 0).astype(jnp.float32)
        match = jnp.where(line == rank, jnp.broadcast_to(hit, (CAP, rows)), 0.0)
        return match, hits

    def weights_of(s, j):
        match, hits = chosen(s, j)
        held = functools.reduce(
            jnp.add, [hits[k] * meta[s, top + k : top + k + 1, :] for k in range(top)]
        )
        return match * held

    def pick(s, slot):
        match = [chosen(s, j)[0] for j in range(local)]
        match = match[0] if local == 1 else jnp.concatenate(match, 0)
        match = match.astype(jnp.bfloat16)
        wide = min(PICK, width)

        def body(k, carry):
            here = pl.ds(pl.multiple_of(k * wide, wide), wide)
            routed[slot, :, here] = jnp.dot(
                match, normed[:, here], preferred_element_type=jnp.float32
            ).astype(jnp.bfloat16)
            return carry

        lax.fori_loop(0, width // wide, body, 0)

    def hid_block(u, zz):
        return hid.at[u, :, cols(zz * 2 + c)]

    def h_copy(u, zz, kind, device):
        return remote(
            hid_block(u, zz), hid_block(u, zz),
            h_send.at[u, zz, kind], h_recv.at[u, zz * 2 + c], device,
        )

    def compute(u):
        p, j = u // local, u % local
        lines_of = pl.ds(pl.multiple_of(j * CAP, CAP), CAP)
        mine = routed[jnp.minimum(p, 1), lines_of, :]
        gate = jnp.dot(mine, wg[j], preferred_element_type=jnp.float32)
        up = jnp.dot(mine, wu[j], preferred_element_type=jnp.float32)
        hid[u, :, cols(t)] = clamped_unit(gate, up).astype(jnp.bfloat16)

        @pl.when(z < chips - 1)
        def _():
            h_copy(u, z, 1, right).start()

        @pl.when(z > 0)
        def _():
            h_copy(u, z, 2, left).start()

        h_copy(u, z, 0, (e, partner)).start()

    def hidden_round(u, k):
        @pl.when(z - k >= 0)
        def _():
            zz = z - k
            h_copy(u, zz, 0, (e, partner)).wait_recv()

            @pl.when(z < chips - 1)
            def _():
                h_copy(u, zz, 1, right).start()

            h_copy(u, zz, 0, (e, partner)).start()

        @pl.when(z + k < chips)
        def _():
            zz = z + k
            h_copy(u, zz, 0, (e, partner)).wait_recv()

            @pl.when(z > 0)
            def _():
                h_copy(u, zz, 2, left).start()

            h_copy(u, zz, 0, (e, partner)).start()

    def hidden_full(u):
        for zz in range(chips):
            other = hid.at[u, :, cols(zz * 2 + 1 - c)]
            remote(
                other, other, h_send.at[u, zz, 0], h_recv.at[u, zz * 2 + 1 - c], (e, partner)
            ).wait_recv()

    def combine(p):
        s = source(p)
        mix = [weights_of(s, j) for j in range(local)]
        mix = mix[0] if local == 1 else jnp.concatenate(mix, 0)
        high = mix.astype(jnp.bfloat16)
        low = (mix - high.astype(jnp.float32)).astype(jnp.bfloat16)
        dims = (((0,), (0,)), ((), ()))
        outs = res[p]
        part[...] = lax.dot_general(
            high, outs, dims, preferred_element_type=jnp.float32
        ) + lax.dot_general(low, outs, dims, preferred_element_type=jnp.float32)

    def ret_copy(p, s, o):
        return remote(ret_out.at[p], ret_in.at[o], r_send.at[p], r_recv.at[o], (s, t))

    def down(i):
        u = piece_of(i)
        p, j = u // local, u % local
        hidden_full(u)
        load_down(i).wait()
        made = jnp.dot(hid[u], wd[i % 2], preferred_element_type=jnp.float32)
        res[p, pl.ds(pl.multiple_of(j * CAP, CAP), CAP), :] = made.astype(jnp.bfloat16)

        @pl.when(i + 2 < pieces)
        def _():
            load_down(i + 2).start()

        @pl.when((p > 0) & (j == local - 1))
        def _():
            combine(p)
            ret_out[p] = part[...].astype(jnp.bfloat16)
            ret_copy(p, source(p), e).start()

    lead = (chips - 1) * LAG + 1
    first_other = local - shift
    first_far = (side + 1) * local - shift
    relays = [(min(k - early, first_other - 1), k) for k in range(early, chips)]
    lasts = [(max(first_far - chips + k, first_other - 1), k) for k in range(chips)]

    def step(i, carry):
        @pl.when(i < pieces)
        def _():
            u = piece_of(i)
            p, j = u // local, u % local

            @pl.when(((j == 0) & (p > 0)) | (i == 0))
            def _():
                s = source(p)
                from_partner(s)
                normalise(s)
                pick(s, jnp.minimum(p, 1))

            @pl.when(i < local)
            def _():
                for copy in load_in(j):
                    copy.wait()

            compute(u)

        for k in range(1, chips):
            ii = i - k * LAG

            @pl.when((ii >= 0) & (ii < pieces))
            def _():
                hidden_round(piece_of(ii), k)

        for act, places in ((relay, relays), (last, lasts)):
            for at in sorted({place for place, _ in places}):

                @pl.when(i == at)
                def _():
                    for place, k in places:
                        if place == at:
                            both(k, act)

        @pl.when(i >= lead)
        def _():
            down(i - lead)

        return carry

    lax.fori_loop(0, pieces + lead, step, 0)

    combine(0)
    total = part[...]
    for i in range(1, n_ep):
        o = (e + i) % n_ep
        ret_copy(i, o, o).wait_recv()
        total = total + ret_in[o].astype(jnp.float32)
    o_ref[...] = total.astype(jnp.bfloat16)

    for p in range(1, n_ep):
        ret_copy(p, source(p), e).wait_send()
        meta_copy(p, e).wait_send()
    for i in range(1, n_tp):
        gb_copy(0, gain_ref, gains, i, t).wait_send()
        gb_copy(1, bias_ref, biases, i, t).wait_send()
    for q in range(SPLIT):
        for zz in range(chips):
            for s in range(n_ep):
                to_partner(block(s, q, zz), s, q, zz).wait_send()

            @pl.when((zz <= z) & (z < chips - 1))
            def _():
                along(block(e, q, zz), q, zz, 0).wait_send()

            @pl.when((zz >= z) & (z > 0))
            def _():
                along(block(e, q, zz), q, zz, 1).wait_send()

            for copy in own_out(block(e, q, zz), q, zz)[:-1]:
                copy.wait_send()
            peers, targets = (row_peers, column_peers)[:: 1 - 2 * (zz % 2)]
            for i, s in enumerate(peers):
                for copy in relayed(i, s, targets, q, zz):
                    copy.wait_send()

    def sent(u, carry):
        for zz in range(chips):
            h_copy(u, zz, 0, (e, partner)).wait_send()

            @pl.when((zz <= z) & (z < chips - 1))
            def _():
                h_copy(u, zz, 1, right).wait_send()

            @pl.when((zz >= z) & (z > 0))
            def _():
                h_copy(u, zz, 2, left).wait_send()

        return carry

    lax.fori_loop(0, pieces, sent, 0)


def on_device(
    n_ep, n_tp,
    tokens, norm_gain, norm_bias, expert_ids, route_weights, gate_weight, up_weight, down_weight,
):
    rows, columns = tokens.shape
    top = expert_ids.shape[1]
    local = gate_weight.shape[0]
    side = math.isqrt(n_ep)
    chips = n_tp // 2
    width = columns * n_tp
    pieces = n_ep * local
    vmem = pl.BlockSpec(memory_space=pltpu.VMEM)
    anywhere = pl.BlockSpec(memory_space=pl.ANY)
    bf16, f32, dma = jnp.bfloat16, jnp.float32, pltpu.SemaphoreType.DMA
    return pl.pallas_call(
        functools.partial(layer_kernel, side, n_tp, top),
        out_shape=jax.ShapeDtypeStruct((rows, columns), bf16),
        in_specs=[vmem] * 5 + [anywhere] * 3,
        out_specs=vmem,
        scratch_shapes=[
            pltpu.VMEM((n_ep, rows, width), bf16),
            pltpu.VMEM((8, rows), f32),
            pltpu.VMEM((n_ep, 8, rows), f32),
            pltpu.VMEM((1, width), f32),
            pltpu.VMEM((1, width), f32),
            pltpu.VMEM((rows, rows), bf16),
            pltpu.VMEM((local, width, columns), bf16),
            pltpu.VMEM((local, width, columns), bf16),
            pltpu.VMEM((2, width, columns), bf16),
            pltpu.VMEM((rows, width), bf16),
            pltpu.VMEM((2, local * CAP, width), bf16),
            pltpu.VMEM((pieces, CAP, width), bf16),
            pltpu.VMEM((n_ep, local * CAP, columns), bf16),
            pltpu.VMEM((rows, columns), f32),
            pltpu.VMEM((n_ep, rows, columns), bf16),
            pltpu.VMEM((n_ep, rows, columns), bf16),
            dma((2, local)),
            dma((2,)),
            dma((SPLIT + 3,)),
            dma((n_ep, SPLIT, chips)),
            dma((SPLIT, chips, 2 * side)),
            dma((side - 1, SPLIT, chips, side - 1)),
            dma((n_ep, SPLIT, n_tp)),
            dma((2, n_tp)),
            dma((2, n_tp)),
            dma((n_ep,)),
            dma((n_ep,)),
            dma((pieces, chips, 3)),
            dma((pieces, n_tp)),
            dma((n_ep,)),
            dma((n_ep,)),
        ],
        compiler_params=pltpu.CompilerParams(
            collective_id=0, has_side_effects=True, vmem_limit_bytes=66_000_000
        ),
    )(
        tokens, norm_gain.reshape(1, columns), norm_bias.reshape(1, columns),
        expert_ids.T, route_weights.T, gate_weight, up_weight, down_weight,
    )


def solution(mesh):
    n_ep, n_tp = mesh.shape["ep"], mesh.shape["tp"]
    placed = (
        P("ep", "tp"),
        P("tp"),
        P("tp"),
        P("ep", None),
        P("ep", None),
        P("ep", None, "tp"),
        P("ep", None, "tp"),
        P("ep", None, "tp"),
    )
    return jax.shard_map(
        functools.partial(on_device, n_ep, n_tp),
        mesh=mesh,
        in_specs=placed,
        out_specs=P("ep", "tp"),
        check_vma=False,
    )
```
